32 devices in a mesh: sp: 8 (over z, x), tp: 4 (over y, core).
Axes of the slice: x: 2, y: 2, z: 4, core: 2. Of those that a mesh axis runs over, the one named last changes fastest.
Arguments:
- tokens: bfloat16 [6144, 2048], P(('sp', 'tp')), may hold values from -6 to 6
- in_gain: float32 [2048], replicated, may hold values from 0.1 to 1.9
- w_query: bfloat16 [2048, 1024], P(None, 'tp'), may hold values from -0.125 to 0.125
- w_key: bfloat16 [2048, 1024], P(None, 'tp'), may hold values from -0.125 to 0.125
- w_value: bfloat16 [2048, 2048], P(None, 'tp'), may hold values from -0.125 to 0.125
- w_input_gate: bfloat16 [2048, 8], replicated, may hold values from -8 to 8
- w_forget_gate: bfloat16 [2048, 8], replicated, may hold values from -0.125 to 0.125
- forget_bias: float32 [8], replicated
- forget_extra: float32 [6144, 8], P('sp', 'tp'), may hold values from -2 to 0
- w_conv_gate: bfloat16 [2048, 2048], P(None, 'tp'), may hold values from -0.125 to 0.125
- w_conv_left: bfloat16 [2048, 2048], P(None, 'tp'), may hold values from -0.125 to 0.125
- w_conv_right: bfloat16 [2048, 2048], P(None, 'tp'), may hold values from -0.125 to 0.125
- conv_taps: float32 [3, 2048], replicated, may hold values from -3.5 to 3.5
- first_memory: float32 [8, 128, 256], P('tp'), may hold values from -2560 to 2560
- first_norm: float32 [8, 128], P('tp'), may hold values from -2560 to 2560
- w_out_memory: bfloat16 [2048, 2048], P('tp'), may hold values from -0.09375 to 0.09375
- w_out_conv: bfloat16 [2048, 2048], P('tp'), may hold values from -0.09375 to 0.09375
Outputs:
- mixed: bfloat16 [6144, 2048], P(('sp', 'tp'))
The draws below stay inside these ranges and needn't reach their ends.
All inputs are finite; a program needn't handle non-finite values.
Results may differ from the reference program's by a relative error of at most 0.015.
The reference program's roundings to bfloat16 on the way count: a program that leaves them out, or rounds other values in their place, can miss the bound.
Values may be sent and summed in bfloat16 or wider, within the bound.
A program may use at most 64 MiB of HBM per device.

```python
import math
import jax
import jax.numpy as jnp
from jax import lax

D = 2048
MEMORY_HEADS = 8
KEY_DIM = 128
VALUE_DIM = 256
CONV_CH = 2048
TAPS = 3
TOK_DEV = 768
SEQUENCE_TOKENS = 6144
QK_WIDTH = 1024
V_WIDTH = 2048
N_TP = 4


def decay_plan(key):
    base_key = jax.random.fold_in(key, 7)
    order_key, spread_key, block_key, place_key, loss_key = jax.random.split(base_key, 5)
    fast_heads = jax.random.permutation(order_key, MEMORY_HEADS) < MEMORY_HEADS // 2
    spread = jax.random.uniform(spread_key, (MEMORY_HEADS,), jnp.float32)
    head_bias = jnp.where(fast_heads, 4.0 + 1.5 * spread, math.log(SEQUENCE_TOKENS) + 1.5 + spread)
    return (head_bias, block_key, place_key, loss_key)


def draw_forget_bias(key, part):
    head_bias, block_key, place_key, loss_key = decay_plan(key)
    return head_bias.astype(jnp.float32)


def draw_forget_extra(key, part):
    head_bias, block_key, place_key, loss_key = decay_plan(key)
    head_rate = jnp.exp(-head_bias)
    factor = jax.random.uniform(block_key, (SEQUENCE_TOKENS // TOK_DEV, MEMORY_HEADS), jnp.float32, 0.0, 2.0)
    block_portion = -jnp.repeat(factor, TOK_DEV, axis=0) * head_rate[None, :]
    place_slots = jax.random.randint(place_key, (3, MEMORY_HEADS), 0, SEQUENCE_TOKENS)
    loss_values = jnp.log(jax.random.uniform(loss_key, (3, MEMORY_HEADS), jnp.float32, 0.6, 0.8))
    token_positions = jnp.arange(SEQUENCE_TOKENS, dtype=jnp.int32)
    span_total_sum = jnp.zeros((SEQUENCE_TOKENS, MEMORY_HEADS), jnp.float32)
    for token_span in range(3):
        span_total_sum = span_total_sum + jnp.where(token_positions[:, None] == place_slots[token_span][None, :], loss_values[token_span][None, :], 0.0)
    return (block_portion + span_total_sum).astype(jnp.float32)


def draw_w_input_gate(key, part):
    weights = jax.random.normal(jax.random.fold_in(key, 11), (D, MEMORY_HEADS), jnp.float32) / math.sqrt(D)
    return jnp.clip(weights, -8.0, 8.0).astype(jnp.bfloat16)


def steps_of(key, extent, cuts, least, top_value):
    loudness, own = 1.0, jax.random.fold_in(key, 6)
    for position, blocks in cuts:
        heights = jnp.exp(jax.random.uniform(jax.random.fold_in(own, position), (blocks,), jnp.float32, least / len(cuts), top_value / len(cuts)))
        loudness = loudness * jnp.repeat(heights, extent[position] // blocks).reshape([-1 if axis == position else 1 for axis in range(len(extent))])
    return loudness


def noise(own_key, shape, scale, bound, pieces=(), held_as=jnp.bfloat16):
    drawn = jax.random.normal(own_key, shape, jnp.float32) * scale
    if len(pieces) > 0:
        drawn = steps_of(own_key, shape, pieces, -0.22, 0.18) * drawn
    return jnp.clip(drawn, min=-bound, max=bound).astype(held_as)


def setup_inputs(seed: int = 0) -> dict:
    splits = jax.random.split(jax.random.key(seed), 18)
    return {
        "tokens": noise(splits[0], (SEQUENCE_TOKENS, D), 1.0, 6.0, ((0, 32),)),
        "in_gain": jnp.clip(1.0 + 0.18 * jax.random.normal(splits[1], (D,), jnp.float32), 0.1, 1.9),
        "w_query": noise(splits[2], (D, QK_WIDTH), D ** -0.5, 0.125, ((1, 4),)),
        "w_key": noise(splits[3], (D, QK_WIDTH), D ** -0.5, 0.125, ((1, 4),)),
        "w_value": noise(splits[4], (D, V_WIDTH), D ** -0.5, 0.125, ((1, 4),)),
        "w_input_gate": draw_w_input_gate(jax.random.fold_in(splits[17], 71), 0),
        "w_forget_gate": noise(splits[6], (D, MEMORY_HEADS), D ** -0.5, 0.125),
        "forget_bias": draw_forget_bias(jax.random.fold_in(splits[17], 71), 0),
        "forget_extra": draw_forget_extra(jax.random.fold_in(splits[17], 71), 0),
        "w_conv_gate": noise(splits[9], (D, CONV_CH), D ** -0.5, 0.125, ((1, 4),)),
        "w_conv_left": noise(splits[10], (D, CONV_CH), D ** -0.5, 0.125, ((1, 4),)),
        "w_conv_right": noise(splits[11], (D, CONV_CH), D ** -0.5, 0.125, ((1, 4),)),
        "conv_taps": noise(splits[12], (TAPS, CONV_CH), TAPS ** -0.5, 3.5, (), jnp.float32),
        "first_memory": noise(splits[13], (MEMORY_HEADS, KEY_DIM, VALUE_DIM), (6 * SEQUENCE_TOKENS ** 0.5), 2560.0, ((0, 4),), jnp.float32),
        "first_norm": noise(splits[14], (MEMORY_HEADS, KEY_DIM), (6 * SEQUENCE_TOKENS ** 0.5), 2560.0, ((0, 4),), jnp.float32),
        "w_out_memory": noise(splits[15], (V_WIDTH, D), (V_WIDTH + CONV_CH) ** -0.5, 0.09375, ((0, 4),)),
        "w_out_conv": noise(splits[16], (CONV_CH, D), (V_WIDTH + CONV_CH) ** -0.5, 0.09375, ((0, 4),)),
    }


epsilon = 1e-06

def rounded(values):
    return lax.optimization_barrier(values.astype(jnp.bfloat16)).astype(jnp.float32)

def mixer_block(carried_state, inputs):
    carry_max, carry_memory, carry_norm = carried_state
    query_rows, key_rows, value_rows, in_pre, log_forget = inputs
    length = query_rows.shape[0]
    query_scale = KEY_DIM ** (-0.5)
    cumulative = jnp.cumsum(log_forget, axis=0)
    decay_total = cumulative[length - 1]
    weight_log = decay_total[None, :] - cumulative + in_pre
    block_max = lax.optimization_barrier(jnp.max(weight_log, axis=0))
    keyed = key_rows.astype(jnp.float32) * jnp.exp(weight_log - block_max[None, :])[:, :, None]
    block_norm = lax.optimization_barrier(jnp.sum(keyed, axis=0))
    block_memory = jnp.einsum('shd,shv->hdv', rounded(keyed), value_rows.astype(jnp.float32))
    token_positions = jnp.arange(length, dtype=jnp.int32)
    causal = token_positions[:, None] >= token_positions[None, :]
    cum_heads = cumulative.T
    log_gap = cum_heads[:, :, None] - cum_heads[:, None, :] + in_pre.T[:, None, :]
    log_gap = jnp.where(causal[None], log_gap, -jnp.inf)
    inter_log = cum_heads + carry_max[:, None]
    row_max = jnp.maximum(inter_log, lax.optimization_barrier(jnp.max(log_gap, axis=2)))
    raw_scores = jnp.einsum('thd,shd->hts', query_rows.astype(jnp.float32), key_rows.astype(jnp.float32)) * query_scale
    mixing = raw_scores * jnp.exp(log_gap - row_max[:, :, None])
    carried = jnp.exp(inter_log - row_max).T
    scaled_query = query_rows.astype(jnp.float32) * query_scale
    from_values = jnp.einsum('hts,shv->thv', rounded(mixing), value_rows.astype(jnp.float32))
    from_memory = jnp.einsum('thd,hdv->thv', scaled_query, carry_memory, precision=lax.Precision.HIGHEST)
    from_norm = jnp.einsum('thd,hd->th', scaled_query, carry_norm, precision=lax.Precision.HIGHEST)
    numerator = from_values + carried[:, :, None] * from_memory
    denominator = lax.optimization_barrier(jnp.sum(mixing, axis=2)).T + carried * from_norm
    memory_out = numerator / jnp.maximum(jnp.abs(denominator), 1.0)[:, :, None]
    row_mean = lax.optimization_barrier(jnp.mean(memory_out * memory_out, axis=(1, 2), keepdims=True))
    heads_out = (memory_out * lax.rsqrt(row_mean + epsilon)).astype(jnp.bfloat16)
    new_max = jnp.maximum(carry_max + decay_total, block_max)
    old_scale = jnp.exp(carry_max + decay_total - new_max)
    new_scale = jnp.exp(block_max - new_max)
    new_memory = old_scale[:, None, None] * carry_memory + new_scale[:, None, None] * block_memory
    new_norm = old_scale[:, None] * carry_norm + new_scale[:, None] * block_norm
    return ((new_max, new_memory, new_norm), heads_out)

def reference(tokens, in_gain, w_query, w_key, w_value, w_input_gate, w_forget_gate, forget_bias, forget_extra, w_conv_gate, w_conv_left, w_conv_right, conv_taps, first_memory, first_norm, w_out_memory, w_out_conv):
    token_rows = tokens.astype(jnp.float32)
    scale_rows = lax.rsqrt(lax.optimization_barrier(jnp.mean(token_rows * token_rows, axis=1, keepdims=True)) + epsilon)
    normed = (token_rows * scale_rows * in_gain).astype(jnp.bfloat16)
    query_rows = jnp.dot(normed, w_query, preferred_element_type=jnp.float32).astype(jnp.bfloat16)
    key_rows = jnp.dot(normed, w_key, preferred_element_type=jnp.float32).astype(jnp.bfloat16)
    value_rows = jnp.dot(normed, w_value, preferred_element_type=jnp.float32).astype(jnp.bfloat16)
    in_pre = jnp.dot(normed, w_input_gate, preferred_element_type=jnp.float32)
    forget_pre = jnp.dot(normed, w_forget_gate, preferred_element_type=jnp.float32) + forget_bias
    log_forget = jax.nn.log_sigmoid(forget_pre) + forget_extra
    conv_gate = rounded(jnp.dot(normed, w_conv_gate, preferred_element_type=jnp.float32))
    conv_left = rounded(jnp.dot(normed, w_conv_left, preferred_element_type=jnp.float32))
    conv_right = rounded(jnp.dot(normed, w_conv_right, preferred_element_type=jnp.float32))
    product = (conv_left * conv_right).astype(jnp.bfloat16)
    padded = jnp.concatenate([jnp.zeros((TAPS - 1, CONV_CH), jnp.bfloat16), product], axis=0).astype(jnp.float32)
    filtered = conv_taps[0][None, :] * padded[0:SEQUENCE_TOKENS]
    for tap_index in range(1, TAPS):
        filtered = filtered + conv_taps[tap_index][None, :] * padded[tap_index:tap_index + SEQUENCE_TOKENS]
    conv_branch = (conv_gate * filtered).astype(jnp.bfloat16)
    blocks = SEQUENCE_TOKENS // TOK_DEV
    inputs = (query_rows.reshape(blocks, TOK_DEV, MEMORY_HEADS, KEY_DIM), key_rows.reshape(blocks, TOK_DEV, MEMORY_HEADS, KEY_DIM), value_rows.reshape(blocks, TOK_DEV, MEMORY_HEADS, VALUE_DIM), in_pre.reshape(blocks, TOK_DEV, MEMORY_HEADS), log_forget.reshape(blocks, TOK_DEV, MEMORY_HEADS))
    start_state = (jnp.zeros((MEMORY_HEADS,), jnp.float32), first_memory, first_norm)
    final_state, heads_out = lax.scan(mixer_block, start_state, inputs)
    heads_out = heads_out.reshape(SEQUENCE_TOKENS, V_WIDTH)
    head_group = V_WIDTH // N_TP
    channel_group = CONV_CH // N_TP
    mixed = jnp.zeros((SEQUENCE_TOKENS, D), jnp.float32)
    for group in range(N_TP):
        head_lo = group * head_group
        channel_lo = group * channel_group
        partial_value = jnp.dot(heads_out[:, head_lo:head_lo + head_group], w_out_memory[head_lo:head_lo + head_group], preferred_element_type=jnp.float32)
        partial_value = partial_value + jnp.dot(conv_branch[:, channel_lo:channel_lo + channel_group], w_out_conv[channel_lo:channel_lo + channel_group], preferred_element_type=jnp.float32)
        mixed = mixed + rounded(partial_value)
    return mixed.astype(jnp.bfloat16)
```

```python
import functools

import jax
import jax.numpy as jnp
from jax import lax
from jax.experimental import pallas as pl
from jax.experimental.pallas import tpu as pltpu
from jax.sharding import PartitionSpec as P

KEY_DIM = 128
VALUE_DIM = 256
TAPS = 3
EPS = 1e-06
NEG = -1e30
MESH = pl.DeviceIdType.MESH
F32 = jnp.float32
BF16 = jnp.bfloat16
AG_CHUNKS = 3
RS_CHUNKS = 4


def mm(a, b):
    return lax.dot_general(a, b, (((1,), (0,)), ((), ())), preferred_element_type=F32)


def mm_t(a, b):
    return lax.dot_general(a, b, (((1,), (1,)), ((), ())), preferred_element_type=F32)


def scan_steps(n):
    steps, d = [], 1
    while d < n:
        steps.append(d)
        d *= 2
    return steps


def kernel(
    n_sp, n_tp, heads, channels, width,
    tokens, gain, wk, wv, wg, wq, wcg, wcl, wcr, bias, extra, taps, first_mem, first_norm,
    wom, woc, out,
    W, WO, XG, PJ, G, COL, NUM, DEN, HC, PROD, halo_out, halo_in,
    A_mem, E_mem, sm_out, sm_in, mem_out_b, mem_in_b, sq_out, sq_in,
    PS, DR, YS, YR,
    w_sem, ag_d, ag_ys, ag_yr, ag_fs, ag_fr, st_s, st_r, hl_s, sq_s, sq_r,
    rd_s, rd_r, ry_s, ry_r,
):
    sp = lax.axis_index("sp")
    tp = lax.axis_index("tp")
    core = lax.rem(tp, 2)
    y = tp // 2
    n_y = n_tp // 2
    partner = tp + 1 - 2 * core
    R, D = tokens.shape
    T = R * n_tp
    qk, vw = heads * KEY_DIM, heads * VALUE_DIM
    o_v, o_g = qk, qk + vw
    o_q = o_g + 128
    o_c = o_q + qk
    total = o_c + 3 * channels
    steps = scan_steps(n_sp)

    srcs = [(wk, 0, qk), (wv, o_v, vw), (wg, o_g, 128), (wq, o_q, qk), (wcg, o_c, channels),
            (wcl, o_c + channels, channels), (wcr, o_c + 2 * channels, channels)]
    w_copies = [
        pltpu.make_async_copy(s, W.at[:, pl.ds(o, n)], w_sem.at[i])
        for i, (s, o, n) in enumerate(srcs)
    ]
    w_copies.append(pltpu.make_async_copy(wom, WO.at[pl.ds(0, vw), :], w_sem.at[7]))
    w_copies.append(pltpu.make_async_copy(woc, WO.at[pl.ds(vw, channels), :], w_sem.at[8]))
    for c in w_copies:
        c.start()

    def rows_of(block, count=1, first=0, n=None):
        n = R * count if n is None else n
        return pl.ds(pl.multiple_of(block * R + first, 16), n)

    x = tokens[...].astype(F32)
    scale = lax.rsqrt(jnp.mean(x * x, axis=1, keepdims=True) + EPS)
    XG[rows_of(tp), :] = (x * scale * gain[...]).astype(BF16)

    def remote(src, dst, ss, rs, to_tp=None, to_sp=None):
        return pltpu.make_async_remote_copy(
            src_ref=src, dst_ref=dst, send_sem=ss, recv_sem=rs,
            device_id=(sp if to_sp is None else to_sp, tp if to_tp is None else to_tp),
            device_id_type=MESH,
        )

    offsets = sorted({d % n_sp for d in steps} | {(n_sp - d) % n_sp for d in steps})
    barrier = pltpu.get_barrier_semaphore()
    for k in range(1, n_tp):
        pl.semaphore_signal(barrier, inc=1, device_id=(sp, lax.rem(tp + k, n_tp)), device_id_type=MESH)
    for k in offsets:
        pl.semaphore_signal(barrier, inc=1, device_id=(lax.rem(sp + k, n_sp), tp), device_id_type=MESH)
    pl.semaphore_wait(barrier, n_tp - 1 + len(offsets))

    sends = []
    piece = R // AG_CHUNKS
    for c in range(AG_CHUNKS):
        for k in range(1, n_y):
            r = rows_of(tp, 1, c * piece, piece)
            cp = remote(XG.at[r, :], XG.at[r, :], ag_ys.at[k - 1, c], ag_yr.at[k - 1, c],
                        to_tp=lax.rem(y + k, n_y) * 2 + core)
            cp.start()
            sends.append(cp)
    own = remote(XG.at[rows_of(tp), :], XG.at[rows_of(tp), :], ag_d.at[0], ag_d.at[1], to_tp=partner)
    own.start()

    tn = 256 if (o_g % 256 == 0 and qk % 256 == 0) else 128

    def project(block, first, last):
        rr = rows_of(block, 2)

        def one(j, _):
            cols = pl.ds(pl.multiple_of(first + j * tn, 128), tn)
            PJ[rr, cols] = mm(XG[rr, :], W[:, cols]).astype(BF16)
            return 0

        lax.fori_loop(0, (last - first) // tn, one, 0)

    def project_gates(block):
        rr = rows_of(block, 2)
        G[rr, :] = mm(XG[rr, :], W[:, o_g:o_g + 128])

    own.wait_recv()
    for c in w_copies[:3]:
        c.wait()
    project(2 * y, 0, o_g)
    project_gates(2 * y)
    for c in w_copies[3:7]:
        c.wait()
    project(2 * y, o_q, total)
    fwd = []
    for c in range(AG_CHUNKS):
        for k in range(1, n_y):
            src = lax.rem(y + n_y - k, n_y) * 2
            r = rows_of(src + core, 1, c * piece, piece)
            remote(XG.at[r, :], XG.at[r, :], ag_ys.at[k - 1, c], ag_yr.at[k - 1, c], to_tp=partner).wait_recv()
            cp = remote(XG.at[r, :], XG.at[r, :], ag_fs.at[k - 1, c], ag_fr.at[k - 1, c], to_tp=partner)
            cp.start()
            sends.append(cp)
    for c in range(AG_CHUNKS):
        for k in range(1, n_y):
            src = lax.rem(y + n_y - k, n_y) * 2
            r = rows_of(src + 1 - core, 1, c * piece, piece)
            remote(XG.at[r, :], XG.at[r, :], ag_fs.at[k - 1, c], ag_fr.at[k - 1, c], to_tp=partner).wait_recv()
    others = [lax.rem(y + k, n_y) * 2 for k in range(1, n_y)]
    for b in others:
        project(b, 0, o_g)
        project_gates(b)

    n_heads = bias.shape[0]
    gt = G[...].T
    in_all, forget_all = gt[0:n_heads], gt[n_heads:2 * n_heads]
    sub = lax.broadcasted_iota(jnp.int32, (n_heads, T), 0)
    sub8 = lax.broadcasted_iota(jnp.int32, (8, T), 0)
    lane = lax.broadcasted_iota(jnp.int32, (8, T), 1)
    in_pre = jnp.zeros((8, T), F32)
    log_f = jnp.zeros((8, T), F32)
    for h in range(heads):
        head = tp * heads + h
        row_i = jnp.sum(jnp.where(sub == head, in_all, 0.0), axis=0, keepdims=True)
        row_f = jnp.sum(jnp.where(sub == head, forget_all, 0.0), axis=0, keepdims=True) + bias[head]
        row_f = jnp.minimum(row_f, 0.0) - jnp.log1p(jnp.exp(-jnp.abs(row_f))) + extra[h:h + 1, :]
        in_pre = jnp.where(sub8 == h, row_i, in_pre)
        log_f = jnp.where(sub8 == h, row_f, log_f)
    cum = log_f
    for d in scan_steps(T):
        cum = cum + jnp.where(lane >= d, pltpu.roll(cum, d, 1), 0.0)
    gap = in_pre - cum
    run = gap
    for d in scan_steps(T):
        run = jnp.maximum(run, jnp.where(lane >= d, pltpu.roll(run, d, 1), run))
    decay = cum[:, T - 1:T]
    gmax = run[:, T - 1:T]
    COL[...] = jnp.concatenate(
        [gap, run, jnp.exp(gap - gmax), jnp.zeros((104, T), F32)], axis=0).T
    ones = jnp.ones((1, 128), F32)

    sm = jnp.zeros((8, 128), F32)
    s8 = lax.broadcasted_iota(jnp.int32, (8, 128), 0)
    for h in range(heads):
        keyed = PJ[:, h * KEY_DIM:(h + 1) * KEY_DIM].astype(F32) * COL[:, 16 + h:17 + h]
        norm = jnp.sum(keyed, axis=0, keepdims=True)
        mem = mm(keyed.T.astype(BF16), PJ[:, o_v + h * VALUE_DIM:o_v + (h + 1) * VALUE_DIM])
        A_mem[h] = mem
        mem_out_b[0, h] = mem.astype(BF16)
        sm = jnp.where(s8 == h, norm, sm)
        sm = jnp.where(s8 == heads + h, decay[h:h + 1] * ones, sm)
        sm = jnp.where(s8 == 2 * heads + h, (decay[h:h + 1] + gmax[h:h + 1]) * ones, sm)
    E_mem[...] = jnp.zeros_like(E_mem)
    sm_out[0] = sm

    def state_copies(i, forward):
        d = steps[i]
        to = lax.rem(sp + d, n_sp)
        return (remote(mem_out_b.at[i], mem_in_b.at[i], st_s.at[i, 0], st_r.at[i, 0], to_sp=to),
                remote(sm_out.at[i], sm_in.at[i], st_s.at[i, 1], st_r.at[i, 1], to_sp=to))

    def state_send(i):
        for cp in state_copies(i, True):
            cp.start()
            sends.append(cp)

    def part(s, j, h):
        return s[j * heads + h:j * heads + h + 1]

    def join(valid, early, early_mem, late, late_mem, h):
        n_e, d_e, m_e = part(early, 0, h), part(early, 1, h), part(early, 2, h)
        n_l, d_l, m_l = part(late, 0, h), part(late, 1, h), part(late, 2, h)
        d_e = jnp.where(valid, d_e, 0.0)
        m_e = jnp.where(valid, m_e, NEG)
        top = jnp.maximum(m_e + d_l, m_l)
        s_e = jnp.where(valid, jnp.exp(m_e + d_l - top), 0.0)
        s_l = jnp.exp(m_l - top)
        return (s_e * n_e + s_l * n_l, d_e + d_l, top,
                s_e[:, 0:1] * early_mem + s_l[:, 0:1] * late_mem)

    state = {"a": sm, "e": jnp.where(s8 >= 2 * heads, NEG, 0.0)}

    def state_step(i):
        for cp in state_copies(i, False):
            cp.wait_recv()
        valid = sp >= steps[i]
        got = sm_in[i]
        last = i + 1 == len(steps)
        for which, ref in (("e", E_mem), ("a", A_mem)):
            if which == "a" and last:
                continue
            new = jnp.zeros((8, 128), F32)
            for h in range(heads):
                n_j, d_j, m_j, mem = join(valid, got, mem_in_b[i, h].astype(F32), state[which], ref[h], h)
                ref[h] = mem
                if which == "a":
                    mem_out_b[i + 1, h] = mem.astype(BF16)
                new = jnp.where(s8 == h, n_j, new)
                new = jnp.where(s8 == heads + h, d_j, new)
                new = jnp.where(s8 == 2 * heads + h, m_j, new)
            state[which] = new
            if which == "a":
                sm_out[i + 1] = new
        if not last:
            state_send(i + 1)

    state_send(0)
    for b in others:
        project(b, o_q, total)

    rb = 256 if T % 256 == 0 else R
    for r0 in range(0, T, rb):
        left = PJ[r0:r0 + rb, o_c + channels:o_c + 2 * channels].astype(F32)
        right = PJ[r0:r0 + rb, o_c + 2 * channels:o_c + 3 * channels].astype(F32)
        prod = (left * right).astype(BF16)
        PROD[8 + r0:8 + r0 + rb, :] = prod.astype(F32)
        if r0 + rb == T:
            halo_out[...] = prod[rb - 16:rb]
    halo = remote(halo_out, halo_in, hl_s.at[0], hl_s.at[1], to_sp=lax.rem(sp + 1, n_sp))
    halo.start()
    sends.append(halo)

    q_scale = KEY_DIM ** -0.5

    def attend(h, r0):
        e = r0 + rb
        q = PJ[r0:e, o_q + h * KEY_DIM:o_q + (h + 1) * KEY_DIM]
        k = PJ[0:e, h * KEY_DIM:(h + 1) * KEY_DIM]
        v = PJ[0:e, o_v + h * VALUE_DIM:o_v + (h + 1) * VALUE_DIM]
        s = mm_t(q, k) * q_scale
        ti = lax.broadcasted_iota(jnp.int32, (rb, e), 0) + r0
        si = lax.broadcasted_iota(jnp.int32, (rb, e), 1)
        w = jnp.where(ti >= si, gap[h:h + 1, 0:e] - COL[r0:e, 8 + h:9 + h], NEG)
        mix = s * jnp.exp(w)
        DEN[h, r0:e, :] = jnp.broadcast_to(jnp.sum(mix, axis=1, keepdims=True), (rb, 128))
        NUM[r0:e, h * VALUE_DIM:(h + 1) * VALUE_DIM] = mm(mix.astype(BF16), v)

    work = [functools.partial(attend, h, r0) for h in range(heads) for r0 in range(0, T, rb)]

    def conv_finish():
        halo.wait_recv()
        before = halo_in[...].astype(F32)[8:16]
        PROD[0:8, :] = jnp.where(sp > 0, before, 0.0)
        tap = taps[:, pl.ds(pl.multiple_of(tp * channels, 128), channels)]
        for r0 in range(0, T, rb):
            f = tap[0:1] * PROD[6 + r0:6 + r0 + rb, :]
            f = f + tap[1:2] * PROD[7 + r0:7 + r0 + rb, :]
            f = f + tap[2:3] * PROD[8 + r0:8 + r0 + rb, :]
            gate = PJ[r0:r0 + rb, o_c:o_c + channels].astype(F32)
            HC[r0:r0 + rb, vw:] = (gate * f).astype(BF16)

    work.append(conv_finish)
    share = -(-len(work) // len(steps))
    for i in range(len(steps)):
        state_step(i)
        if i + 1 < len(steps):
            for w_ in work[:share]:
                w_()
            work = work[share:]
        elif work:
            for w_ in work:
                w_()

    e_s = state["e"]
    sq = [jnp.zeros((rb, 1), F32) for _ in range(T // rb)]
    for h in range(heads):
        n_e, d_e, m_e = part(e_s, 0, h), part(e_s, 1, h), part(e_s, 2, h)
        cmax = jnp.maximum(m_e, d_e)
        s_p, s_f = jnp.exp(m_e - cmax), jnp.exp(d_e - cmax)
        c_mem = s_p[:, 0:1] * E_mem[h] + s_f[:, 0:1] * first_mem[h]
        c_norm = s_p * n_e + s_f * first_norm[h:h + 1, :]
        hi = c_mem.astype(BF16)
        lo = (c_mem - hi.astype(F32)).astype(BF16)
        for b, r0 in enumerate(range(0, T, rb)):
            e = r0 + rb
            q = PJ[r0:e, o_q + h * KEY_DIM:o_q + (h + 1) * KEY_DIM]
            fm = mm(q, hi) + mm(q, lo)
            fn = jnp.sum(q.astype(F32) * c_norm, axis=1, keepdims=True)
            m0 = COL[r0:e, 8 + h:9 + h]
            m = jnp.maximum(m0, cmax[:, 0:1])
            k0 = jnp.exp(m0 - m)
            k1 = jnp.exp(cmax[:, 0:1] - m) * q_scale
            den = k0 * DEN[h, r0:e, 0:1] + k1 * fn
            inv = 1.0 / jnp.maximum(jnp.abs(den), 1.0)
            cols = slice(h * VALUE_DIM, (h + 1) * VALUE_DIM)
            mo = (k0 * NUM[r0:e, cols] + k1 * fm) * inv
            NUM[r0:e, cols] = mo
            sq[b] = sq[b] + jnp.sum(mo * mo, axis=1, keepdims=True)
    sq_col = jnp.concatenate([jnp.broadcast_to(s, (rb, 128)) for s in sq], axis=0)
    mine = sq_col.T[0:8]
    sq_out[...] = mine
    for k in range(1, n_tp):
        cp = remote(sq_out, sq_in.at[k - 1], sq_s.at[k - 1], sq_r.at[k - 1], to_tp=lax.rem(tp + k, n_tp))
        cp.start()
        sends.append(cp)
    tot = mine
    for k in range(1, n_tp):
        remote(sq_out, sq_in.at[k - 1], sq_s.at[k - 1], sq_r.at[k - 1], to_tp=partner).wait_recv()
        tot = tot + sq_in[k - 1]
    r_scale = lax.rsqrt(tot / float(width) + EPS)
    COL[...] = jnp.concatenate([r_scale] * 16, axis=0).T
    for r0 in range(0, T, rb):
        HC[r0:r0 + rb, 0:vw] = (NUM[r0:r0 + rb, :] * COL[r0:r0 + rb, 0:1]).astype(BF16)

    for c in w_copies[7:]:
        c.wait()
    cw = D // RS_CHUNKS

    def out_block(chip_row, idx, j):
        cols = pl.ds(pl.multiple_of(j * cw, 128), cw)
        rr = rows_of(chip_row, 2)
        PS[rr, cols] = mm(HC[rr, :], WO[:, cols]).astype(BF16)
        return remote(PS.at[rows_of(chip_row + 1 - core), cols], DR.at[idx, :, cols],
                      rd_s.at[idx, j], rd_r.at[idx, j], to_tp=partner)

    def pair_sum(chip_row, idx, j):
        cols = pl.ds(pl.multiple_of(j * cw, 128), cw)
        mine_rows = rows_of(chip_row + core)
        remote(PS.at[mine_rows, cols], DR.at[idx, :, cols], rd_s.at[idx, j], rd_r.at[idx, j],
               to_tp=partner).wait_recv()
        return cols, PS[mine_rows, cols].astype(F32) + DR[idx, :, cols].astype(F32)

    def y_copy(k, j):
        cols = pl.ds(pl.multiple_of(j * cw, 128), cw)
        return remote(YS.at[k - 1, :, cols], YR.at[k - 1, :, cols], ry_s.at[k - 1, j], ry_r.at[k - 1, j],
                      to_tp=lax.rem(y + k, n_y) * 2 + core)

    for k in range(1, n_y):
        def one(j, _, k=k):
            @pl.when(j < RS_CHUNKS)
            def _():
                out_block(others[k - 1], k, j).start()

            @pl.when(j > 0)
            def _():
                cols, s = pair_sum(others[k - 1], k, j - 1)
                YS[k - 1, :, cols] = s.astype(BF16)
                y_copy(k, j - 1).start()
            return 0

        lax.fori_loop(0, RS_CHUNKS + 1, one, 0)

    def local(j, _):
        out_block(2 * y, 0, j).start()
        return 0

    lax.fori_loop(0, RS_CHUNKS, local, 0)

    def finish(j, _):
        cols, s = pair_sum(2 * y, 0, j)
        for k in range(1, n_y):
            y_copy(k, j).wait_recv()
            s = s + YR[k - 1, :, cols].astype(F32)
        out[:, cols] = s.astype(BF16)
        return 0

    lax.fori_loop(0, RS_CHUNKS, finish, 0)

    for cp in sends:
        cp.wait_send()
    own.wait_send()

    def drain(j, _):
        for idx in range(n_y):
            cols = pl.ds(pl.multiple_of(j * cw, 128), cw)
            remote(PS.at[rows_of(2 * y + core), cols], DR.at[idx, :, cols], rd_s.at[idx, j],
                   rd_r.at[idx, j], to_tp=partner).wait_send()
        for k in range(1, n_y):
            y_copy(k, j).wait_send()
        return 0

    lax.fori_loop(0, RS_CHUNKS, drain, 0)


def per_device(
    n_sp, n_tp,
    tokens, in_gain, w_query, w_key, w_value, w_input_gate, w_forget_gate, forget_bias,
    forget_extra, w_conv_gate, w_conv_left, w_conv_right, conv_taps, first_memory, first_norm,
    w_out_memory, w_out_conv,
):
    heads = w_query.shape[1] // KEY_DIM
    channels = w_conv_gate.shape[1]
    R, D = tokens.shape
    T = R * n_tp
    n_y = n_tp // 2
    qk, vw = heads * KEY_DIM, heads * VALUE_DIM
    total = 2 * qk + vw + 128 + 3 * channels
    n_heads = w_input_gate.shape[1]
    gates = jnp.concatenate(
        [w_input_gate, w_forget_gate, jnp.zeros((D, 128 - 2 * n_heads), BF16)], axis=1)
    n_st = len(scan_steps(n_sp))
    vmem = pl.BlockSpec(memory_space=pltpu.VMEM)
    hbm = pl.BlockSpec(memory_space=pl.ANY)
    V, dma = pltpu.VMEM, pltpu.SemaphoreType.DMA
    ny1 = n_y - 1
    return pl.pallas_call(
        functools.partial(kernel, n_sp, n_tp, heads, channels, n_heads * VALUE_DIM),
        out_shape=jax.ShapeDtypeStruct((R, D), BF16),
        in_specs=[vmem, vmem] + [hbm] * 7
        + [pl.BlockSpec(memory_space=pltpu.SMEM)] + [vmem] * 4 + [hbm] * 2,
        out_specs=vmem,
        scratch_shapes=[
            V((D, total), BF16), V((vw + channels, D), BF16), V((T, D), BF16), V((T, total), BF16),
            V((T, 128), F32), V((T, 128), F32), V((T, vw), F32), V((heads, T, 128), F32),
            V((T, vw + channels), BF16), V((8 + T, channels), F32),
            V((16, channels), BF16), V((16, channels), BF16),
            V((heads, KEY_DIM, VALUE_DIM), F32), V((heads, KEY_DIM, VALUE_DIM), F32),
            V((n_st, 8, 128), F32), V((n_st, 8, 128), F32),
            V((n_st, heads, KEY_DIM, VALUE_DIM), BF16), V((n_st, heads, KEY_DIM, VALUE_DIM), BF16),
            V((8, T), F32), V((n_tp - 1, 8, T), F32),
            V((T, D), BF16), V((n_y, R, D), BF16), V((ny1, R, D), BF16), V((ny1, R, D), BF16),
            dma((9,)), dma((2,)), dma((ny1, AG_CHUNKS)), dma((ny1, AG_CHUNKS)),
            dma((ny1, AG_CHUNKS)), dma((ny1, AG_CHUNKS)), dma((n_st, 2)), dma((n_st, 2)), dma((2,)),
            dma((n_tp - 1,)), dma((n_tp - 1,)),
            dma((n_y, RS_CHUNKS)), dma((n_y, RS_CHUNKS)), dma((ny1, RS_CHUNKS)), dma((ny1, RS_CHUNKS)),
        ],
        compiler_params=pltpu.CompilerParams(
            collective_id=0, has_side_effects=True, vmem_limit_bytes=60 * 1024 * 1024),
        name="layer",
    )(
        tokens, in_gain.reshape(1, D), w_key, w_value, gates, w_query, w_conv_gate, w_conv_left,
        w_conv_right, forget_bias, forget_extra.T, conv_taps, first_memory, first_norm,
        w_out_memory, w_out_conv,
    )


def solution(mesh):
    in_specs = (
        P(("sp", "tp"), None), P(), P(None, "tp"), P(None, "tp"), P(None, "tp"), P(), P(), P(),
        P("sp", "tp"), P(None, "tp"), P(None, "tp"), P(None, "tp"), P(), P("tp", None, None),
        P("tp", None), P("tp", None), P("tp", None),
    )
    return jax.shard_map(
        functools.partial(per_device, mesh.shape["sp"], mesh.shape["tp"]),
        mesh=mesh, in_specs=in_specs, out_specs=P(("sp", "tp"), None), check_vma=False,
    )
```

```python
import functools

import jax
import jax.numpy as jnp
from jax import lax
from jax.experimental import pallas as pl
from jax.experimental.pallas import tpu as pltpu
from jax.sharding import PartitionSpec as P

KEY_DIM = 128
VALUE_DIM = 256
TAPS = 3
EPS = 1e-06
NEG = -1e30
MESH = pl.DeviceIdType.MESH
F32 = jnp.float32
BF16 = jnp.bfloat16
AG_CHUNKS = 3
RS_CHUNKS = 4


def mm(a, b):
    return lax.dot_general(a, b, (((1,), (0,)), ((), ())), preferred_element_type=F32)


def mm_t(a, b):
    return lax.dot_general(a, b, (((1,), (1,)), ((), ())), preferred_element_type=F32)


def scan_steps(n):
    steps, d = [], 1
    while d < n:
        steps.append(d)
        d *= 2
    return steps


def kernel(
    n_sp, n_tp, heads, channels, width,
    tokens, gain, wk, wv, wq, wcg, wcl, wcr, wig, wfg, bias, extra, taps, first_mem, first_norm,
    wom, woc, out,
    W, WO, XG, PJ, G, COL, NUM, DEN, HC, PROD, halo_out, halo_in,
    A_mem, E_mem, sm_out, sm_in, mem_out_b, mem_in_b, sq_out, sq_in,
    PS, DR, YS, YR,
    w_sem, ag_d, ag_ys, ag_yr, ag_fs, ag_fr, st_s, st_r, hl_s, sq_s, sq_r,
    rd_s, rd_r, ry_s, ry_r,
):
    sp = lax.axis_index("sp")
    tp = lax.axis_index("tp")
    core = lax.rem(tp, 2)
    y = tp // 2
    n_y = n_tp // 2
    partner = tp + 1 - 2 * core
    R, D = tokens.shape
    T = R * n_tp
    qk, vw = heads * KEY_DIM, heads * VALUE_DIM
    o_v, o_g = qk, qk + vw
    o_q = o_g + 128
    o_c = o_q + qk
    total = o_c + 3 * channels
    steps = scan_steps(n_sp)

    srcs = [(wk, 0, qk), (wv, o_v, vw), (wq, o_q, qk), (wcg, o_c, channels),
            (wcl, o_c + channels, channels), (wcr, o_c + 2 * channels, channels)]
    w_copies = [
        pltpu.make_async_copy(s, W.at[:, pl.ds(o, n)], w_sem.at[i])
        for i, (s, o, n) in enumerate(srcs)
    ]
    w_copies.append(pltpu.make_async_copy(wom, WO.at[pl.ds(0, vw), :], w_sem.at[6]))
    w_copies.append(pltpu.make_async_copy(woc, WO.at[pl.ds(vw, channels), :], w_sem.at[7]))
    for c in w_copies:
        c.start()

    def rows_of(block, count=1, first=0, n=None):
        n = R * count if n is None else n
        return pl.ds(pl.multiple_of(block * R + first, 16), n)

    x = tokens[...].astype(F32)
    scale = lax.rsqrt(jnp.mean(x * x, axis=1, keepdims=True) + EPS)
    XG[rows_of(tp), :] = (x * scale * gain[...]).astype(BF16)

    def remote(src, dst, ss, rs, to_tp=None, to_sp=None):
        return pltpu.make_async_remote_copy(
            src_ref=src, dst_ref=dst, send_sem=ss, recv_sem=rs,
            device_id=(sp if to_sp is None else to_sp, tp if to_tp is None else to_tp),
            device_id_type=MESH,
        )

    offsets = sorted({d % n_sp for d in steps} | {(n_sp - d) % n_sp for d in steps})
    barrier = pltpu.get_barrier_semaphore()
    for k in range(1, n_tp):
        pl.semaphore_signal(barrier, inc=1, device_id=(sp, lax.rem(tp + k, n_tp)), device_id_type=MESH)
    for k in offsets:
        pl.semaphore_signal(barrier, inc=1, device_id=(lax.rem(sp + k, n_sp), tp), device_id_type=MESH)
    pl.semaphore_wait(barrier, n_tp - 1 + len(offsets))

    sends = []
    piece = R // AG_CHUNKS
    for c in range(AG_CHUNKS):
        for k in range(1, n_y):
            r = rows_of(tp, 1, c * piece, piece)
            cp = remote(XG.at[r, :], XG.at[r, :], ag_ys.at[k - 1, c], ag_yr.at[k - 1, c],
                        to_tp=lax.rem(y + k, n_y) * 2 + core)
            cp.start()
            sends.append(cp)
    own = remote(XG.at[rows_of(tp), :], XG.at[rows_of(tp), :], ag_d.at[0], ag_d.at[1], to_tp=partner)
    own.start()

    tn = 256 if (o_g % 256 == 0 and qk % 256 == 0) else 128

    def project(block, first, last):
        rr = rows_of(block, 2)

        def one(j, _):
            cols = pl.ds(pl.multiple_of(first + j * tn, 128), tn)
            PJ[rr, cols] = mm(XG[rr, :], W[:, cols]).astype(BF16)
            return 0

        lax.fori_loop(0, (last - first) // tn, one, 0)

    def project_gates(block):
        rr = rows_of(block, 2)
        G[rr, :] = mm(XG[rr, :], W[:, o_g:o_g + 128])

    n_heads = bias.shape[0]
    W[:, o_g:o_g + 128] = jnp.concatenate(
        [wig[...].astype(F32), wfg[...].astype(F32), jnp.zeros((128 - 2 * n_heads, D), F32)],
        axis=0).T.astype(BF16)
    own.wait_recv()
    for c in w_copies[:2]:
        c.wait()
    project(2 * y, 0, o_g)
    project_gates(2 * y)
    for c in w_copies[2:6]:
        c.wait()
    project(2 * y, o_q, total)
    fwd = []
    for c in range(AG_CHUNKS):
        for k in range(1, n_y):
            src = lax.rem(y + n_y - k, n_y) * 2
            r = rows_of(src + core, 1, c * piece, piece)
            remote(XG.at[r, :], XG.at[r, :], ag_ys.at[k - 1, c], ag_yr.at[k - 1, c], to_tp=partner).wait_recv()
            cp = remote(XG.at[r, :], XG.at[r, :], ag_fs.at[k - 1, c], ag_fr.at[k - 1, c], to_tp=partner)
            cp.start()
            sends.append(cp)
    for c in range(AG_CHUNKS):
        for k in range(1, n_y):
            src = lax.rem(y + n_y - k, n_y) * 2
            r = rows_of(src + 1 - core, 1, c * piece, piece)
            remote(XG.at[r, :], XG.at[r, :], ag_fs.at[k - 1, c], ag_fr.at[k - 1, c], to_tp=partner).wait_recv()
    others = [lax.rem(y + k, n_y) * 2 for k in range(1, n_y)]
    for b in others:
        project(b, 0, o_g)
        project_gates(b)

    gt = G[...].T
    in_all, forget_all = gt[0:n_heads], gt[n_heads:2 * n_heads]
    sub = lax.broadcasted_iota(jnp.int32, (n_heads, T), 0)
    sub8 = lax.broadcasted_iota(jnp.int32, (8, T), 0)
    lane = lax.broadcasted_iota(jnp.int32, (8, T), 1)
    in_pre = jnp.zeros((8, T), F32)
    log_f = jnp.zeros((8, T), F32)
    for h in range(heads):
        head = tp * heads + h
        row_i = jnp.sum(jnp.where(sub == head, in_all, 0.0), axis=0, keepdims=True)
        row_f = jnp.sum(jnp.where(sub == head, forget_all, 0.0), axis=0, keepdims=True) + bias[head]
        row_f = jnp.minimum(row_f, 0.0) - jnp.log1p(jnp.exp(-jnp.abs(row_f))) + extra[h:h + 1, :]
        in_pre = jnp.where(sub8 == h, row_i, in_pre)
        log_f = jnp.where(sub8 == h, row_f, log_f)
    cum = log_f
    for d in scan_steps(T):
        cum = cum + jnp.where(lane >= d, pltpu.roll(cum, d, 1), 0.0)
    gap = in_pre - cum
    decay = cum[:, T - 1:T]
    gmax = jnp.max(gap, axis=1, keepdims=True)
    COL[...] = jnp.concatenate([jnp.exp(gap - gmax), jnp.zeros((120, T), F32)], axis=0).T
    ones = jnp.ones((1, 128), F32)
    s8 = lax.broadcasted_iota(jnp.int32, (8, 128), 0)

    def state_copies(i, h):
        to = lax.rem(sp + steps[i], n_sp)
        return (remote(mem_out_b.at[i, h], mem_in_b.at[i, h], st_s.at[i, h, 0], st_r.at[i, h, 0], to_sp=to),
                remote(sm_out.at[i, h], sm_in.at[i, h], st_s.at[i, h, 1], st_r.at[i, h, 1], to_sp=to))

    def state_send(i, h, vec, mem):
        n, d, m = vec
        mem_out_b[i, h] = mem.astype(BF16)
        sm_out[i, h] = jnp.where(s8 == 0, n, jnp.where(s8 == 1, d, m))
        for cp in state_copies(i, h):
            cp.start()
            sends.append(cp)

    zero = jnp.zeros((1, 128), F32)
    incl, excl = [None] * heads, [(zero, zero, jnp.full((1, 128), NEG, F32))] * heads
    for h in range(heads):
        keyed = PJ[:, h * KEY_DIM:(h + 1) * KEY_DIM].astype(F32) * COL[:, h:h + 1]
        norm = jnp.sum(keyed, axis=0, keepdims=True)
        mem = mm(keyed.T.astype(BF16), PJ[:, o_v + h * VALUE_DIM:o_v + (h + 1) * VALUE_DIM])
        A_mem[h] = mem
        incl[h] = (norm, decay[h:h + 1] * ones, (decay[h:h + 1] + gmax[h:h + 1]) * ones)
        state_send(0, h, incl[h], mem)
    E_mem[...] = jnp.zeros_like(E_mem)

    def join(valid, early, early_mem, late, late_mem):
        n_e, d_e, m_e = early
        n_l, d_l, m_l = late
        d_e = jnp.where(valid, d_e, 0.0)
        m_e = jnp.where(valid, m_e, NEG)
        top = jnp.maximum(m_e + d_l, m_l)
        s_e = jnp.where(valid, jnp.exp(m_e + d_l - top), 0.0)
        s_l = jnp.exp(m_l - top)
        return ((s_e * n_e + s_l * n_l, d_e + d_l, top),
                s_e[:, 0:1] * early_mem + s_l[:, 0:1] * late_mem)

    def state_step(i, h):
        for cp in state_copies(i, h):
            cp.wait_recv()
        valid = sp >= steps[i]
        got = sm_in[i, h]
        early = (got[0:1], got[1:2], got[2:3])
        early_mem = mem_in_b[i, h].astype(F32)
        if i + 1 < len(steps):
            incl[h], mem = join(valid, early, early_mem, incl[h], A_mem[h])
            A_mem[h] = mem
            state_send(i + 1, h, incl[h], mem)
        excl[h], mem = join(valid, early, early_mem, excl[h], E_mem[h])
        E_mem[h] = mem

    def work_running_max():
        run = gap
        for d in scan_steps(T):
            run = jnp.maximum(run, jnp.where(lane >= d, pltpu.roll(run, d, 1), run))
        COL[...] = jnp.concatenate([run, jnp.zeros((120, T), F32)], axis=0).T

    rb = 256 if T % 256 == 0 else R

    def work_project(first, last):
        for b in others:
            project(b, first, last)

    halo = remote(halo_out, halo_in, hl_s.at[0], hl_s.at[1], to_sp=lax.rem(sp + 1, n_sp))

    def work_product():
        for r0 in range(0, T, rb):
            left = PJ[r0:r0 + rb, o_c + channels:o_c + 2 * channels].astype(F32)
            right = PJ[r0:r0 + rb, o_c + 2 * channels:o_c + 3 * channels].astype(F32)
            prod = (left * right).astype(BF16)
            PROD[8 + r0:8 + r0 + rb, :] = prod.astype(F32)
            if r0 + rb == T:
                halo_out[...] = prod[rb - 16:rb]
        halo.start()
        sends.append(halo)

    q_scale = KEY_DIM ** -0.5

    def attend(h, r0):
        e = r0 + rb
        q = PJ[r0:e, o_q + h * KEY_DIM:o_q + (h + 1) * KEY_DIM]
        k = PJ[0:e, h * KEY_DIM:(h + 1) * KEY_DIM]
        v = PJ[0:e, o_v + h * VALUE_DIM:o_v + (h + 1) * VALUE_DIM]
        s = mm_t(q, k) * q_scale
        ti = lax.broadcasted_iota(jnp.int32, (rb, e), 0) + r0
        si = lax.broadcasted_iota(jnp.int32, (rb, e), 1)
        w = jnp.where(ti >= si, gap[h:h + 1, 0:e] - COL[r0:e, h:h + 1], NEG)
        mix = s * jnp.exp(w)
        DEN[h, r0:e, :] = jnp.broadcast_to(jnp.sum(mix, axis=1, keepdims=True), (rb, 128))
        NUM[r0:e, h * VALUE_DIM:(h + 1) * VALUE_DIM] = mm(mix.astype(BF16), v)

    work = [functools.partial(attend, h, r0) for h in range(heads) for r0 in range(0, T, rb)]

    def conv_finish():
        halo.wait_recv()
        before = halo_in[...].astype(F32)[8:16]
        PROD[0:8, :] = jnp.where(sp > 0, before, 0.0)
        tap = taps[:, pl.ds(pl.multiple_of(tp * channels, 128), channels)]
        for r0 in range(0, T, rb):
            f = tap[0:1] * PROD[6 + r0:6 + r0 + rb, :]
            f = f + tap[1:2] * PROD[7 + r0:7 + r0 + rb, :]
            f = f + tap[2:3] * PROD[8 + r0:8 + r0 + rb, :]
            gate = PJ[r0:r0 + rb, o_c:o_c + channels].astype(F32)
            HC[r0:r0 + rb, vw:] = (gate * f).astype(BF16)

    c1 = o_c + channels
    slots = [
        [functools.partial(work_project, o_q, c1), work_running_max],
        [functools.partial(work_project, c1, total)],
        [work_product, work.pop(0)],
    ]
    events = [(i, h) for i in range(len(steps)) for h in range(heads)]
    rest = work + [conv_finish]
    for n, event in enumerate(events[:-heads]):
        for w_ in (slots.pop(0) if slots else [rest.pop(0)] if rest else []):
            w_()
        state_step(*event)
    for group in slots:
        for w_ in group:
            w_()
    for w_ in rest:
        w_()

    sq = [jnp.zeros((rb, 1), F32) for _ in range(T // rb)]
    for h in range(heads):
        state_step(len(steps) - 1, h)
        n_e, d_e, m_e = excl[h]
        cmax = jnp.maximum(m_e, d_e)
        s_p, s_f = jnp.exp(m_e - cmax), jnp.exp(d_e - cmax)
        c_mem = s_p[:, 0:1] * E_mem[h] + s_f[:, 0:1] * first_mem[h]
        c_norm = s_p * n_e + s_f * first_norm[h:h + 1, :]
        hi = c_mem.astype(BF16)
        lo = (c_mem - hi.astype(F32)).astype(BF16)
        for b, r0 in enumerate(range(0, T, rb)):
            e = r0 + rb
            q = PJ[r0:e, o_q + h * KEY_DIM:o_q + (h + 1) * KEY_DIM]
            fm = mm(q, hi) + mm(q, lo)
            fn = jnp.sum(q.astype(F32) * c_norm, axis=1, keepdims=True)
            m0 = COL[r0:e, h:h + 1]
            m = jnp.maximum(m0, cmax[:, 0:1])
            k0 = jnp.exp(m0 - m)
            k1 = jnp.exp(cmax[:, 0:1] - m) * q_scale
            den = k0 * DEN[h, r0:e, 0:1] + k1 * fn
            inv = 1.0 / jnp.maximum(jnp.abs(den), 1.0)
            cols = slice(h * VALUE_DIM, (h + 1) * VALUE_DIM)
            mo = (k0 * NUM[r0:e, cols] + k1 * fm) * inv
            NUM[r0:e, cols] = mo
            sq[b] = sq[b] + jnp.sum(mo * mo, axis=1, keepdims=True)
    sq_col = jnp.concatenate([jnp.broadcast_to(s, (rb, 128)) for s in sq], axis=0)
    mine = sq_col.T[0:8]
    sq_out[...] = mine
    for k in range(1, n_tp):
        cp = remote(sq_out, sq_in.at[k - 1], sq_s.at[k - 1], sq_r.at[k - 1], to_tp=lax.rem(tp + k, n_tp))
        cp.start()
        sends.append(cp)
    tot = mine
    for k in range(1, n_tp):
        remote(sq_out, sq_in.at[k - 1], sq_s.at[k - 1], sq_r.at[k - 1], to_tp=partner).wait_recv()
        tot = tot + sq_in[k - 1]
    r_scale = lax.rsqrt(tot / float(width) + EPS)
    COL[...] = jnp.concatenate([r_scale] * 16, axis=0).T
    for r0 in range(0, T, rb):
        HC[r0:r0 + rb, 0:vw] = (NUM[r0:r0 + rb, :] * COL[r0:r0 + rb, 0:1]).astype(BF16)

    for c in w_copies[6:]:
        c.wait()
    cw = D // RS_CHUNKS

    def out_block(chip_row, idx, j):
        cols = pl.ds(pl.multiple_of(j * cw, 128), cw)
        rr = rows_of(chip_row, 2)
        PS[rr, cols] = mm(HC[rr, :], WO[:, cols]).astype(BF16)
        return remote(PS.at[rows_of(chip_row + 1 - core), cols], DR.at[idx, :, cols],
                      rd_s.at[idx, j], rd_r.at[idx, j], to_tp=partner)

    def pair_sum(chip_row, idx, j):
        cols = pl.ds(pl.multiple_of(j * cw, 128), cw)
        mine_rows = rows_of(chip_row + core)
        remote(PS.at[mine_rows, cols], DR.at[idx, :, cols], rd_s.at[idx, j], rd_r.at[idx, j],
               to_tp=partner).wait_recv()
        return cols, PS[mine_rows, cols].astype(F32) + DR[idx, :, cols].astype(F32)

    def y_copy(k, j):
        cols = pl.ds(pl.multiple_of(j * cw, 128), cw)
        return remote(YS.at[k - 1, :, cols], YR.at[k - 1, :, cols], ry_s.at[k - 1, j], ry_r.at[k - 1, j],
                      to_tp=lax.rem(y + k, n_y) * 2 + core)

    for k in range(1, n_y):
        def one(j, _, k=k):
            @pl.when(j < RS_CHUNKS)
            def _():
                out_block(others[k - 1], k, j).start()

            @pl.when(j > 0)
            def _():
                cols, s = pair_sum(others[k - 1], k, j - 1)
                YS[k - 1, :, cols] = s.astype(BF16)
                y_copy(k, j - 1).start()
            return 0

        lax.fori_loop(0, RS_CHUNKS + 1, one, 0)

    def local(j, _):
        out_block(2 * y, 0, j).start()
        return 0

    lax.fori_loop(0, RS_CHUNKS, local, 0)

    def finish(j, _):
        cols, s = pair_sum(2 * y, 0, j)
        for k in range(1, n_y):
            y_copy(k, j).wait_recv()
            s = s + YR[k - 1, :, cols].astype(F32)
        out[:, cols] = s.astype(BF16)
        return 0

    lax.fori_loop(0, RS_CHUNKS, finish, 0)

    for cp in sends:
        cp.wait_send()
    own.wait_send()

    def drain(j, _):
        for idx in range(n_y):
            cols = pl.ds(pl.multiple_of(j * cw, 128), cw)
            remote(PS.at[rows_of(2 * y + core), cols], DR.at[idx, :, cols], rd_s.at[idx, j],
                   rd_r.at[idx, j], to_tp=partner).wait_send()
        for k in range(1, n_y):
            y_copy(k, j).wait_send()
        return 0

    lax.fori_loop(0, RS_CHUNKS, drain, 0)


def per_device(
    n_sp, n_tp,
    tokens, in_gain, w_query, w_key, w_value, w_input_gate, w_forget_gate, forget_bias,
    forget_extra, w_conv_gate, w_conv_left, w_conv_right, conv_taps, first_memory, first_norm,
    w_out_memory, w_out_conv,
):
    heads = w_query.shape[1] // KEY_DIM
    channels = w_conv_gate.shape[1]
    R, D = tokens.shape
    T = R * n_tp
    n_y = n_tp // 2
    qk, vw = heads * KEY_DIM, heads * VALUE_DIM
    total = 2 * qk + vw + 128 + 3 * channels
    n_heads = w_input_gate.shape[1]
    n_st = len(scan_steps(n_sp))
    vmem = pl.BlockSpec(memory_space=pltpu.VMEM)
    hbm = pl.BlockSpec(memory_space=pl.ANY)
    V, dma = pltpu.VMEM, pltpu.SemaphoreType.DMA
    ny1 = n_y - 1
    return pl.pallas_call(
        functools.partial(kernel, n_sp, n_tp, heads, channels, n_heads * VALUE_DIM),
        out_shape=jax.ShapeDtypeStruct((R, D), BF16),
        in_specs=[vmem, vmem] + [hbm] * 6 + [vmem] * 2
        + [pl.BlockSpec(memory_space=pltpu.SMEM)] + [vmem] * 4 + [hbm] * 2,
        out_specs=vmem,
        scratch_shapes=[
            V((D, total), BF16), V((vw + channels, D), BF16), V((T, D), BF16), V((T, total), BF16),
            V((T, 128), F32), V((T, 128), F32), V((T, vw), F32), V((heads, T, 128), F32),
            V((T, vw + channels), BF16), V((8 + T, channels), F32),
            V((16, channels), BF16), V((16, channels), BF16),
            V((heads, KEY_DIM, VALUE_DIM), F32), V((heads, KEY_DIM, VALUE_DIM), F32),
            V((n_st, heads, 8, 128), F32), V((n_st, heads, 8, 128), F32),
            V((n_st, heads, KEY_DIM, VALUE_DIM), BF16), V((n_st, heads, KEY_DIM, VALUE_DIM), BF16),
            V((8, T), F32), V((n_tp - 1, 8, T), F32),
            V((T, D), BF16), V((n_y, R, D), BF16), V((ny1, R, D), BF16), V((ny1, R, D), BF16),
            dma((8,)), dma((2,)), dma((ny1, AG_CHUNKS)), dma((ny1, AG_CHUNKS)),
            dma((ny1, AG_CHUNKS)), dma((ny1, AG_CHUNKS)), dma((n_st, heads, 2)), dma((n_st, heads, 2)), dma((2,)),
            dma((n_tp - 1,)), dma((n_tp - 1,)),
            dma((n_y, RS_CHUNKS)), dma((n_y, RS_CHUNKS)), dma((ny1, RS_CHUNKS)), dma((ny1, RS_CHUNKS)),
        ],
        compiler_params=pltpu.CompilerParams(
            collective_id=0, has_side_effects=True, vmem_limit_bytes=60 * 1024 * 1024),
        name="layer",
    )(
        tokens, in_gain.reshape(1, D), w_key, w_value, w_query, w_conv_gate, w_conv_left,
        w_conv_right, w_input_gate.T, w_forget_gate.T, forget_bias, forget_extra.T, conv_taps, first_memory, first_norm,
        w_out_memory, w_out_conv,
    )


def solution(mesh):
    in_specs = (
        P(("sp", "tp"), None), P(), P(None, "tp"), P(None, "tp"), P(None, "tp"), P(), P(), P(),
        P("sp", "tp"), P(None, "tp"), P(None, "tp"), P(None, "tp"), P(), P("tp", None, None),
        P("tp", None), P("tp", None), P("tp", None),
    )
    return jax.shard_map(
        functools.partial(per_device, mesh.shape["sp"], mesh.shape["tp"]),
        mesh=mesh, in_specs=in_specs, out_specs=P(("sp", "tp"), None), check_vma=False,
    )
```
